32 devices in a mesh: sp: 8 (over z, x), dp: 4 (over y, core).
Axes of the slice: x: 2, y: 2, z: 4, core: 2. Of those that a mesh axis runs over, the one named last changes fastest.
Arguments:
- hidden_in: bfloat16 [4, 1024, 2048], P('dp', 'sp'), may hold values from -6 to 6
- in_weight: bfloat16 [2048, 512], P(('sp', 'dp')), may hold values from -0.125 to 0.125
- lam_real: float32 [32, 64], replicated, may hold values from -4 to 0, as said below
- lam_imag: float32 [32, 64], replicated, may hold values from 1 to 200
- log_step: float32 [32], replicated, may hold values from -4.61 to -2.3
- b_real: float32 [32, 64, 16], replicated, may hold values from -1 to 1
- b_imag: float32 [32, 64, 16], replicated, may hold values from -1 to 1
- c_real: float32 [32, 16, 64], replicated, may hold values from -0.3 to 0.3
- c_imag: float32 [32, 16, 64], replicated, may hold values from -0.3 to 0.3
- skip_weight: float32 [512], replicated, may hold values from -4 to 4
- lin_weight: bfloat16 [512, 2048], P(None, ('sp', 'dp')), may hold values from -0.25 to 0.25
- gate_weight: bfloat16 [512, 2048], P(None, ('sp', 'dp')), may hold values from -0.25 to 0.25
Outputs:
- mixed: bfloat16 [4, 1024, 2048], P('dp', 'sp')
The draws below stay inside these ranges and needn't reach their ends.
Inputs may be any that keep to these rules, and one draw needn't show every extreme that they name: `lam_real`: negative in every entry.
All inputs are finite; a program needn't handle non-finite values.
Results may differ from the reference program's by a relative error of at most 0.0047.
The reference program's roundings to bfloat16 on the way (of `inputs` and `mixer_out`) count: a program that leaves them out, or rounds other values in their place, can miss the bound.
Values may be sent and summed in bfloat16 or wider, within the bound.
A program may use at most 64 MiB of HBM per device.

```python
import math
import jax
import jax.numpy as jnp
from jax import lax

D = 2048
GROUPS = 32
CH_GROUP = 16
STATES = 64
U = 512
LEN = 1024
BATCH = 4


def decay_plan(key):
    base = jax.random.fold_in(key, 11)
    first, second, third, fourth = jax.random.split(base, 4)
    log_step = jax.random.uniform(first, (GROUPS,), jnp.float32, math.log(0.01), math.log(0.1))
    share = 0.5
    quick = jax.random.uniform(second, (GROUPS,), jnp.float32) < share
    quick_rate = jnp.exp(jax.random.uniform(third, (GROUPS, STATES), jnp.float32, math.log(1.0 / 100.0), math.log(1.0 / 30.0)))
    slow_rate = jnp.exp(jax.random.uniform(fourth, (GROUPS, STATES), jnp.float32, math.log(0.2 / LEN), math.log(2.0 / LEN)))
    rate = jnp.where(quick[:, None], quick_rate, slow_rate)
    lam_real = -rate / jnp.exp(log_step)[:, None]
    return (lam_real, log_step)


def draw_lam_real(key, part):
    return decay_plan(key)[0]


def draw_log_step(key, part):
    return decay_plan(key)[1]


def shard_levels(key, dims, cuts, low, largest):
    def one(dim, parts):
        steps = jax.random.uniform(jax.random.fold_in(jax.random.fold_in(key, 6), dim), (parts,), jnp.float32, low / len(cuts), largest / len(cuts))
        return jnp.repeat(jnp.exp(steps), dims[dim] // parts).reshape((-1,) + (1,) * (len(dims) - dim - 1))

    factor_of = one(*cuts[0])
    for cut in cuts[1:]:
        factor_of = factor_of * one(*cut)
    return factor_of


def noise(key, extent, spread, reach, cuts=(), kind=jnp.bfloat16):
    drawn = jax.random.normal(key, extent, jnp.float32) * spread
    if len(cuts) > 0:
        drawn = shard_levels(key, extent, cuts, -0.22, 0.18) * drawn
    return jnp.clip(drawn, min=-reach, max=reach).astype(kind)


def setup_inputs(seed: int = 0) -> dict:
    key_of = jax.random.split(jax.random.key(seed), 13)
    return {
        "hidden_in": noise(key_of[0], (BATCH, LEN, D), 1.0, 6.0, ((0, 4), (1, 8))),
        "in_weight": noise(key_of[1], (D, U), D ** -0.5, 0.125, ((0, 32),)),
        "lam_real": draw_lam_real(jax.random.fold_in(key_of[12], 71), 0),
        "lam_imag": jnp.clip(jax.random.uniform(key_of[3], (GROUPS, STATES), jnp.float32, 1.0, 200.0), 1.0, 200.0),
        "log_step": draw_log_step(jax.random.fold_in(key_of[12], 71), 0),
        "b_real": noise(key_of[5], (GROUPS, STATES, CH_GROUP), (2 * CH_GROUP) ** -0.5, 1.0, (), jnp.float32),
        "b_imag": noise(key_of[6], (GROUPS, STATES, CH_GROUP), (2 * CH_GROUP) ** -0.5, 1.0, (), jnp.float32),
        "c_real": noise(key_of[7], (GROUPS, CH_GROUP, STATES), 0.05, 0.3, (), jnp.float32),
        "c_imag": noise(key_of[8], (GROUPS, CH_GROUP, STATES), 0.05, 0.3, (), jnp.float32),
        "skip_weight": noise(key_of[9], (U,), 1.0, 4.0, (), jnp.float32),
        "lin_weight": noise(key_of[10], (U, D), U ** -0.5, 0.25, ((1, 32),)),
        "gate_weight": noise(key_of[11], (U, D), U ** -0.5, 0.25, ((1, 32),)),
    }


def step_factors(lam_real, lam_imag, log_step, b_real, b_imag):
    step = jnp.exp(log_step)[:, None]
    xpart = lam_real * step
    wpart = lam_imag * step
    decay_re = jnp.exp(xpart) * jnp.cos(wpart)
    decay_im = jnp.exp(xpart) * jnp.sin(wpart)
    numer_re = jnp.expm1(xpart) * jnp.cos(wpart) - 2.0 * jnp.sin(0.5 * wpart) ** 2
    numer_im = decay_im
    magnitude = lam_real * lam_real + lam_imag * lam_imag
    ratio_re = (numer_re * lam_real + numer_im * lam_imag) / magnitude
    ratio_im = (numer_im * lam_real - numer_re * lam_imag) / magnitude
    bbar_re = ratio_re[..., None] * b_real - ratio_im[..., None] * b_imag
    bbar_im = ratio_re[..., None] * b_imag + ratio_im[..., None] * b_real
    return decay_re, decay_im, bbar_re, bbar_im


def combine(left, right):
    lre, lim, lbre, lbim = left
    rre, rim, rbre, rbim = right
    return (rre * lre - rim * lim, rre * lim + rim * lre,
            rre * lbre - rim * lbim + rbre, rre * lbim + rim * lbre + rbim)


def reference(hidden_in, in_weight, lam_real, lam_imag, log_step, b_real, b_imag, c_real, c_imag, skip_weight, lin_weight, gate_weight):
    highest = lax.Precision.HIGHEST
    flat = hidden_in.reshape(BATCH * LEN, D)
    inputs = jnp.dot(flat, in_weight, preferred_element_type=jnp.float32).astype(jnp.bfloat16)
    inputs = inputs.reshape(BATCH, LEN, U)
    decay_re, decay_im, bbar_re, bbar_im = step_factors(lam_real, lam_imag, log_step, b_real, b_imag)
    lanes = GROUPS * STATES
    flat_re = decay_re.reshape(lanes)
    flat_im = decay_im.reshape(lanes)
    block = math.gcd(LEN, 512)

    def one_sequence(sequence):
        blocks = sequence.reshape(LEN // block, block, U)

        def block_step(carry, piece):
            carry_re, carry_im = carry
            source = piece.astype(jnp.float32)
            shaped = source.reshape(block, GROUPS, CH_GROUP)
            drive_re = jnp.einsum('tgh,gph->tgp', shaped, bbar_re, precision=highest).reshape(block, lanes)
            drive_im = jnp.einsum('tgh,gph->tgp', shaped, bbar_im, precision=highest).reshape(block, lanes)
            are = jnp.broadcast_to(flat_re, drive_re.shape)
            aim = jnp.broadcast_to(flat_im, drive_re.shape)
            cum_re, cum_im, local_re, local_im = lax.associative_scan(combine, (are, aim, drive_re, drive_im), axis=0)
            state_re = local_re + cum_re * carry_re - cum_im * carry_im
            state_im = local_im + cum_re * carry_im + cum_im * carry_re
            summed = (jnp.einsum('tgp,ghp->tgh', state_re.reshape(block, GROUPS, STATES), c_real, precision=highest)
                      - jnp.einsum('tgp,ghp->tgh', state_im.reshape(block, GROUPS, STATES), c_imag, precision=highest))
            result = jax.nn.gelu(summed.reshape(block, U) + skip_weight * source)
            return (state_re[-1], state_im[-1]), result.astype(jnp.bfloat16)

        zeros = jnp.zeros((lanes,), jnp.float32)
        _, results = lax.scan(block_step, (zeros, zeros), blocks)
        return results.reshape(LEN, U)

    mixer_out = lax.map(one_sequence, inputs).reshape(BATCH * LEN, U)
    linear = jnp.dot(mixer_out, lin_weight, preferred_element_type=jnp.float32)
    gate = jnp.dot(mixer_out, gate_weight, preferred_element_type=jnp.float32)
    mixed = (linear * jax.nn.sigmoid(gate)).astype(jnp.bfloat16)
    return mixed.reshape(BATCH, LEN, D)
```

```python
import functools

import jax
import jax.numpy as jnp
from jax import lax
from jax.experimental import pallas as pl
from jax.experimental.pallas import tpu as pltpu
from jax.sharding import PartitionSpec as P

MESH = pl.DeviceIdType.MESH
LANES = 128
SUBLANES = 8
CORES = 2


def step_factors(lam_real, lam_imag, log_step):
    step = jnp.exp(log_step)[:, None]
    xpart = lam_real * step
    wpart = lam_imag * step
    decay_re = jnp.exp(xpart) * jnp.cos(wpart)
    decay_im = jnp.exp(xpart) * jnp.sin(wpart)
    numer_re = jnp.expm1(xpart) * jnp.cos(wpart) - 2.0 * jnp.sin(0.5 * wpart) ** 2
    magnitude = lam_real * lam_real + lam_imag * lam_imag
    ratio_re = (numer_re * lam_real + decay_im * lam_imag) / magnitude
    ratio_im = (decay_im * lam_real - numer_re * lam_imag) / magnitude
    return decay_re, decay_im, ratio_re, ratio_im


def cmul(a, b):
    return a[0] * b[0] - a[1] * b[1], a[0] * b[1] + a[1] * b[0]


def cpow(a, power):
    result = None
    while power:
        if power & 1:
            result = a if result is None else cmul(result, a)
        power >>= 1
        if power:
            a = cmul(a, a)
    return result


def split(value):
    high = value.astype(jnp.bfloat16)
    return high, (value - high.astype(jnp.float32)).astype(jnp.bfloat16)


def nn(a, b):
    return jnp.dot(a, b, preferred_element_type=jnp.float32)


def nt(a, b):
    return lax.dot_general(a, b, (((1,), (1,)), ((), ())), preferred_element_type=jnp.float32)


def kernel(
    sizes,
    x_ref,
    win_ref,
    wout_ref,
    factor_ref,
    bmat_ref,
    cmat_ref,
    skip_ref,
    out_ref,
    win,
    wout,
    blocks,
    drive,
    ends,
    edge,
    mine,
    others,
    inner,
    send_z,
    recv_z,
    send_a,
    recv_a,
    send_b,
    recv_b,
    send_c,
    recv_c,
    send_e,
    recv_e,
):
    sp, dp = sizes
    n = dp // CORES
    nz = sp // n
    sp_me, dp_me = lax.axis_index("sp"), lax.axis_index("dp")
    z, x = sp_me // n, sp_me % n
    y, core = dp_me // CORES, dp_me % CORES
    rows = win_ref.shape[0]
    cols = wout_ref.shape[1]
    tokens, width = x_ref.shape
    channels = win_ref.shape[1]
    heads, lanes = bmat_ref.shape[1:]
    steps = tokens // SUBLANES

    def place(dz, a, b):
        zz = (z + dz) % nz
        xx = (x + a * (1 - core) + b * core) % n
        yy = (y + b * (1 - core) + a * core) % n
        return zz * n + xx, yy * CORES + core

    def owner(dz, a, b, c):
        zz = (z + nz - dz) % nz
        xx = (x + n - (a * (1 - c) + b * c)) % n
        yy = (y + n - (b * (1 - c) + a * c)) % n
        return (zz * n + xx) * dp + yy * CORES + c

    partner = (sp_me, y * CORES + (1 - core))

    def slot(w, index):
        if w == 0:
            return win.at[pl.ds(pl.multiple_of(index * rows, rows), rows), :]
        return wout.at[:, pl.ds(pl.multiple_of(index * cols, cols), cols), :]

    def copy(w, dz, a, b, c, target, sems, where, own=False):
        index = owner(dz, a, b, c)
        there = slot(w, index)
        source = (win_ref, wout_ref)[w] if own else there
        spot = (w,) + where
        return pltpu.make_async_remote_copy(
            src_ref=source,
            dst_ref=there,
            send_sem=sems[0].at[spot],
            recv_sem=sems[1].at[spot],
            device_id=target,
            device_id_type=MESH,
        )

    zs, as_, bs, cs = (send_z, recv_z), (send_a, recv_a), (send_b, recv_b), (send_c, recv_c)

    def copy_z(w, dz):
        return copy(w, 0, 0, 0, core, place(dz, 0, 0), zs, (dz - 1,), own=True)

    def copy_a(w, a, dz):
        return copy(w, dz, 0, 0, core, place(0, a, 0), as_, (a - 1, dz), own=dz == 0)

    def copy_b(w, b, a, dz):
        return copy(w, dz, a, 0, core, place(0, 0, b), bs, (b - 1, a, dz), own=dz == 0 and a == 0)

    def copy_c(w, b, a, dz):
        return copy(w, dz, a, b, core, partner, cs, (b, a, dz), own=dz == 0 and a == 0 and b == 0)

    def arrive_z(w, dz):
        copy(w, dz, 0, 0, core, partner, zs, (dz - 1,)).wait_recv()

    def arrive_a(w, a, dz):
        copy(w, dz, a, 0, core, partner, as_, (a - 1, dz)).wait_recv()

    def arrive_b(w, b, a, dz):
        copy(w, dz, a, b, core, partner, bs, (b - 1, a, dz)).wait_recv()

    def arrive_c(w, b, a, dz):
        copy(w, dz, a, b, 1 - core, partner, cs, (b, a, dz)).wait_recv()

    def pass_b(w, a, dz):
        for b in range(1, n):
            copy_b(w, b, a, dz).start()
        copy_c(w, 0, a, dz).start()

    def pass_a(w, dz):
        for a in range(1, n):
            copy_a(w, a, dz).start()
        pass_b(w, 0, dz)

    def phase_own(w):
        for dz in range(1, nz):
            copy_z(w, dz).start()
        pass_a(w, 0)

    def phase_z(w):
        for dz in range(1, nz):
            arrive_z(w, dz)
            pass_a(w, dz)

    def phase_a(w):
        for a in range(1, n):
            for dz in range(nz):
                arrive_a(w, a, dz)
                pass_b(w, a, dz)

    def phase_b(w):
        for b in range(1, n):
            for a in range(n):
                for dz in range(nz):
                    arrive_b(w, b, a, dz)
                    copy_c(w, b, a, dz).start()

    def phase_c(w):
        for b in range(n):
            for a in range(n):
                for dz in range(nz):
                    arrive_c(w, b, a, dz)

    def close(w):
        for dz in range(1, nz):
            copy_z(w, dz).wait_send()
        for dz in range(nz):
            for a in range(n):
                if a > 0:
                    copy_a(w, a, dz).wait_send()
                for b in range(n):
                    if b > 0:
                        copy_b(w, b, a, dz).wait_send()
                    copy_c(w, b, a, dz).wait_send()

    barrier = pltpu.get_barrier_semaphore()
    greeted = [((sp_me + j) % sp, dp_me) for j in range(1, sp)]
    greeted += [(sp_me, (y + j) % n * CORES + core) for j in range(1, n)]
    greeted += [partner]
    for device in greeted:
        pl.semaphore_signal(barrier, inc=1, device_id=device, device_id_type=MESH)
    pl.semaphore_wait(barrier, len(greeted))

    phase_own(0)
    phase_own(1)
    home = sp_me * dp + dp_me
    win[pl.ds(pl.multiple_of(home * rows, rows), rows), :] = win_ref[...]
    wout[:, pl.ds(pl.multiple_of(home * cols, cols), cols), :] = wout_ref[...]
    phase_z(0)

    share = LANES // heads
    count = channels // LANES
    wide = lanes // count
    deep = wide // share

    def block(ref, part, i, base):
        piece = ref[part, :, i * wide : (i + 1) * wide]
        lane = lax.broadcasted_iota(jnp.int32, piece.shape, 1)
        stacked = [
            jnp.where((lane >= g * deep) & (lane < (g + 1) * deep), piece, 0.0)
            for g in range(share)
        ]
        high, low = split(jnp.concatenate(stacked, axis=0))
        blocks[base + 2 * part, i] = high
        blocks[base + 2 * part + 1, i] = low

    for i in range(count):
        for part in range(2):
            block(bmat_ref, part, i, 0)
    phase_a(0)
    for i in range(count):
        for part in range(2):
            block(cmat_ref, part, i, 4)
    phase_b(0)
    phase_z(1)
    phase_c(0)

    high_k = width // 4
    total = nn(x_ref[:, :high_k], win[:high_k, :])
    for i in range(1, 4):
        span = slice(i * high_k, (i + 1) * high_k)
        total += nn(x_ref[:, span], win[span, :])
    inputs = total.astype(jnp.bfloat16)

    r = lax.broadcasted_iota(jnp.int32, (tokens, tokens), 0)
    c = lax.broadcasted_iota(jnp.int32, (tokens, tokens), 1)
    order = lambda v: (v & (SUBLANES - 1)) * steps + lax.shift_right_logical(v, 3)
    mix = jnp.where(c == order(r), 1.0, 0.0).astype(jnp.bfloat16)
    back = jnp.where(r == order(c), 1.0, 0.0).astype(jnp.bfloat16)
    source = nn(mix, inputs)
    spread = source.astype(jnp.bfloat16)

    decay = (factor_ref[0:1, :], factor_ref[1:2, :])
    for i in range(count):
        span = slice(i * wide, (i + 1) * wide)
        piece = spread[:, i * LANES : (i + 1) * LANES]
        for part in range(2):
            drive[part, :, span] = nn(piece, blocks[2 * part, i]) + nn(piece, blocks[2 * part + 1, i])
        shape = (SUBLANES, wide)
        mul = (jnp.broadcast_to(decay[0][:, span], shape), jnp.broadcast_to(decay[1][:, span], shape))
        state = (drive[0, :SUBLANES, span], drive[1, :SUBLANES, span])
        for k in range(1, steps):
            at = slice(k * SUBLANES, (k + 1) * SUBLANES)
            moved = cmul(mul, state)
            state = (moved[0] + drive[0, at, span], moved[1] + drive[1, at, span])
        ends[0, :, span] = state[0]
        ends[1, :, span] = state[1]

    jump = cpow(decay, steps)
    carry = (ends[0, 0:1, :], ends[1, 0:1, :])
    for s in range(1, SUBLANES):
        moved = cmul(jump, carry)
        carry = (moved[0] + ends[0, s : s + 1, :], moved[1] + ends[1, s : s + 1, :])
    mine[0:1, :] = carry[0]
    mine[1:2, :] = carry[1]

    def exchange(j):
        return pltpu.make_async_remote_copy(
            src_ref=mine,
            dst_ref=others.at[j - 1],
            send_sem=send_e.at[j - 1],
            recv_sem=recv_e.at[j - 1],
            device_id=((sp_me + j) % sp, dp_me),
            device_id_type=MESH,
        )

    for j in range(1, sp):
        exchange(j).start()
    phase_a(1)
    phase_b(1)
    far = cpow(decay, tokens)
    carry = (jnp.zeros_like(decay[0]), jnp.zeros_like(decay[0]))
    for j in range(1, sp):
        exchange(j).wait_recv()
    for j in range(sp - 1, 0, -1):
        moved = cmul(far, carry)
        before = sp_me >= j
        carry = (
            jnp.where(before, moved[0] + others[j - 1, 0:1, :], 0.0),
            jnp.where(before, moved[1] + others[j - 1, 1:2, :], 0.0),
        )
    edge[0, 0:1, :] = carry[0]
    edge[1, 0:1, :] = carry[1]
    for s in range(1, SUBLANES):
        moved = cmul(jump, carry)
        carry = (moved[0] + ends[0, s - 1 : s, :], moved[1] + ends[1, s - 1 : s, :])
        edge[0, s : s + 1, :] = carry[0]
        edge[1, s : s + 1, :] = carry[1]

    for i in range(count):
        span = slice(i * wide, (i + 1) * wide)
        shape = (SUBLANES, wide)
        mul = (jnp.broadcast_to(decay[0][:, span], shape), jnp.broadcast_to(decay[1][:, span], shape))
        state = (edge[0, :, span], edge[1, :, span])
        for k in range(steps):
            at = slice(k * SUBLANES, (k + 1) * SUBLANES)
            moved = cmul(mul, state)
            state = (moved[0] + drive[0, at, span], moved[1] + drive[1, at, span])
            drive[0, at, span] = state[0]
            drive[1, at, span] = state[1]
        summed = []
        for part in range(2):
            high, low = split(drive[part, :, span])
            c_high, c_low = blocks[4 + 2 * part, i], blocks[5 + 2 * part, i]
            summed.append(nt(high, c_high) + (nt(low, c_high) + nt(high, c_low)))
        here = slice(i * LANES, (i + 1) * LANES)
        result = jax.nn.gelu(summed[0] - summed[1] + skip_ref[:, here] * source[:, here])
        inner[:, here] = result.astype(jnp.bfloat16)

    mixer_out = nn(back, inner[...]).astype(jnp.bfloat16)
    phase_c(1)
    tile = 2 * LANES
    for i in range(width // tile):
        span = slice(i * tile, (i + 1) * tile)
        linear = nt(mixer_out, wout[0, span, :])
        gate = nt(mixer_out, wout[1, span, :])
        out_ref[:, span] = (linear * jax.nn.sigmoid(gate)).astype(jnp.bfloat16)

    for j in range(1, sp):
        exchange(j).wait_send()
    close(0)
    close(1)


def shards(
    sizes,
    hidden_in,
    in_weight,
    lam_real,
    lam_imag,
    log_step,
    b_real,
    b_imag,
    c_real,
    c_imag,
    skip_weight,
    lin_weight,
    gate_weight,
):
    sp, dp = sizes
    n = dp // CORES
    nz = sp // n
    tokens, width = hidden_in.shape[1:]
    rows, channels = in_weight.shape
    groups, states, heads = b_real.shape
    lanes = groups * states
    decay_re, decay_im, ratio_re, ratio_im = step_factors(lam_real, lam_imag, log_step)
    factor = jnp.stack((decay_re.reshape(lanes), decay_im.reshape(lanes)), 0)
    bbar_re = ratio_re[..., None] * b_real - ratio_im[..., None] * b_imag
    bbar_im = ratio_re[..., None] * b_imag + ratio_im[..., None] * b_real
    bmat = jnp.stack((bbar_re, bbar_im), 0).transpose(0, 3, 1, 2).reshape(2, heads, lanes)
    cmat = jnp.stack((c_real, c_imag), 0).transpose(0, 2, 1, 3).reshape(2, heads, lanes)
    pieces = jnp.stack((lin_weight.T, gate_weight.T), 0)
    count = channels // LANES
    bf16, f32 = jnp.bfloat16, jnp.float32
    pair = lambda *shape: [pltpu.SemaphoreType.DMA(shape)] * 2
    mixed = pl.pallas_call(
        functools.partial(kernel, sizes),
        out_shape=jax.ShapeDtypeStruct((tokens, width), bf16),
        in_specs=[pl.BlockSpec(memory_space=pltpu.VMEM)] * 7,
        out_specs=pl.BlockSpec(memory_space=pltpu.VMEM),
        scratch_shapes=[
            pltpu.VMEM((rows * sp * dp, channels), bf16),
            pltpu.VMEM((2, width, channels), bf16),
            pltpu.VMEM((8, count, LANES, lanes // count), bf16),
            pltpu.VMEM((2, tokens, lanes), f32),
            pltpu.VMEM((2, SUBLANES, lanes), f32),
            pltpu.VMEM((2, SUBLANES, lanes), f32),
            pltpu.VMEM((2, lanes), f32),
            pltpu.VMEM((sp - 1, 2, lanes), f32),
            pltpu.VMEM((tokens, channels), bf16),
            *pair(2, nz - 1),
            *pair(2, n - 1, nz),
            *pair(2, n - 1, n, nz),
            *pair(2, n, n, nz),
            *pair(sp - 1),
        ],
        compiler_params=pltpu.CompilerParams(
            collective_id=0, has_side_effects=True, vmem_limit_bytes=60 * 1024 * 1024
        ),
    )(hidden_in[0], in_weight, pieces, factor, bmat, cmat, skip_weight[None])
    return mixed[None]


def solution(mesh):
    sizes = (mesh.shape["sp"], mesh.shape["dp"])
    placed = (
        P("dp", "sp", None),
        P(("sp", "dp"), None),
        P(),
        P(),
        P(),
        P(),
        P(),
        P(),
        P(),
        P(),
        P(None, ("sp", "dp")),
        P(None, ("sp", "dp")),
    )
    return jax.shard_map(
        functools.partial(shards, sizes),
        mesh=mesh,
        in_specs=placed,
        out_specs=P("dp", "sp", None),
        check_vma=False,
    )
```

```python
import functools

import jax
import jax.numpy as jnp
from jax import lax
from jax.experimental import pallas as pl
from jax.experimental.pallas import tpu as pltpu
from jax.sharding import PartitionSpec as P

MESH = pl.DeviceIdType.MESH
LANES = 128
SUBLANES = 8
CORES = 2


def expm1(value):
    series = jnp.ones_like(value)
    for k in range(11, 1, -1):
        series = 1.0 + series * value * (1.0 / k)
    return jnp.where(jnp.abs(value) < 0.5, value * series, jnp.exp(value) - 1.0)


def step_factors(lam_real, lam_imag, step):
    xpart = lam_real * step
    wpart = lam_imag * step
    decay_re = jnp.exp(xpart) * jnp.cos(wpart)
    decay_im = jnp.exp(xpart) * jnp.sin(wpart)
    numer_re = expm1(xpart) * jnp.cos(wpart) - 2.0 * jnp.sin(0.5 * wpart) ** 2
    magnitude = lam_real * lam_real + lam_imag * lam_imag
    ratio_re = (numer_re * lam_real + decay_im * lam_imag) / magnitude
    ratio_im = (decay_im * lam_real - numer_re * lam_imag) / magnitude
    return decay_re, decay_im, ratio_re, ratio_im


def cmul(a, b):
    return a[0] * b[0] - a[1] * b[1], a[0] * b[1] + a[1] * b[0]


def cpow(a, power):
    result = None
    while power:
        if power & 1:
            result = a if result is None else cmul(result, a)
        power >>= 1
        if power:
            a = cmul(a, a)
    return result


def split(value):
    high = value.astype(jnp.bfloat16)
    return high, (value - high.astype(jnp.float32)).astype(jnp.bfloat16)


def nn(a, b):
    return jnp.dot(a, b, preferred_element_type=jnp.float32)


def nt(a, b):
    return lax.dot_general(a, b, (((1,), (1,)), ((), ())), preferred_element_type=jnp.float32)


def kernel(
    sizes,
    x_ref,
    win_ref,
    wout_ref,
    lam_re_ref,
    lam_im_ref,
    log_step_ref,
    b_re_ref,
    b_im_ref,
    c_re_ref,
    c_im_ref,
    skip_ref,
    out_ref,
    win,
    wout,
    tables,
    factor,
    compact,
    drive,
    ends,
    edge,
    mine,
    others,
    inner,
    send_z,
    recv_z,
    send_a,
    recv_a,
    send_b,
    recv_b,
    send_c,
    recv_c,
    send_e,
    recv_e,
):
    sp, dp = sizes
    n = dp // CORES
    nz = sp // n
    sp_me, dp_me = lax.axis_index("sp"), lax.axis_index("dp")
    z, x = sp_me // n, sp_me % n
    y, core = dp_me // CORES, dp_me % CORES
    rows = win_ref.shape[0]
    cols = wout_ref.shape[1]
    tokens, width = x_ref.shape
    channels = win_ref.shape[1]
    groups, heads, states = c_re_ref.shape
    lanes = groups * states
    steps = tokens // SUBLANES

    def across(dz, sign):
        if nz & (nz - 1):
            return (z + nz + sign * dz) % nz
        total = 0
        bit = 1
        while bit < nz:
            held = z // bit % 2
            total = total + bit * (1 - held if dz & bit else held)
            bit *= 2
        return total

    def place(dz, a, b):
        zz = across(dz, 1)
        xx = (x + a * (1 - core) + b * core) % n
        yy = (y + b * (1 - core) + a * core) % n
        return zz * n + xx, yy * CORES + core

    def owner(dz, a, b, c):
        zz = across(dz, -1)
        xx = (x + n - (a * (1 - c) + b * c)) % n
        yy = (y + n - (b * (1 - c) + a * c)) % n
        return (zz * n + xx) * dp + yy * CORES + c

    partner = (sp_me, y * CORES + (1 - core))

    def slot(w, index):
        if w == 0:
            return win.at[pl.ds(pl.multiple_of(index * rows, rows), rows), :]
        return wout.at[:, pl.ds(pl.multiple_of(index * cols, cols), cols), :]

    def copy(w, dz, a, b, c, target, sems, where, own=False):
        index = owner(dz, a, b, c)
        there = slot(w, index)
        source = (win_ref, wout_ref)[w] if own else there
        spot = (w,) + where
        return pltpu.make_async_remote_copy(
            src_ref=source,
            dst_ref=there,
            send_sem=sems[0].at[spot],
            recv_sem=sems[1].at[spot],
            device_id=target,
            device_id_type=MESH,
        )

    zs, as_, bs, cs = (send_z, recv_z), (send_a, recv_a), (send_b, recv_b), (send_c, recv_c)

    def copy_z(w, dz):
        return copy(w, 0, 0, 0, core, place(dz, 0, 0), zs, (dz - 1,), own=True)

    def copy_a(w, a, dz):
        return copy(w, dz, 0, 0, core, place(0, a, 0), as_, (a - 1, dz), own=dz == 0)

    def copy_b(w, b, a, dz):
        return copy(w, dz, a, 0, core, place(0, 0, b), bs, (b - 1, a, dz), own=dz == 0 and a == 0)

    def copy_c(w, b, a, dz):
        return copy(w, dz, a, b, core, partner, cs, (b, a, dz), own=dz == 0 and a == 0 and b == 0)

    def arrive_z(w, dz):
        copy(w, dz, 0, 0, core, partner, zs, (dz - 1,)).wait_recv()

    def arrive_a(w, a, dz):
        copy(w, dz, a, 0, core, partner, as_, (a - 1, dz)).wait_recv()

    def arrive_b(w, b, a, dz):
        copy(w, dz, a, b, core, partner, bs, (b - 1, a, dz)).wait_recv()

    def arrive_c(w, b, a, dz):
        copy(w, dz, a, b, 1 - core, partner, cs, (b, a, dz)).wait_recv()

    def pass_b(w, a, dz):
        for b in range(1, n):
            copy_b(w, b, a, dz).start()
        copy_c(w, 0, a, dz).start()

    def pass_a(w, dz):
        for a in range(1, n):
            copy_a(w, a, dz).start()
        pass_b(w, 0, dz)

    def phase_own(w):
        for dz in range(1, nz):
            copy_z(w, dz).start()
        pass_a(w, 0)

    def step_z(w, dz):
        arrive_z(w, dz)
        pass_a(w, dz)

    def step_a(w, a, dz):
        arrive_a(w, a, dz)
        pass_b(w, a, dz)

    def step_b(w, b, a, dz):
        arrive_b(w, b, a, dz)
        copy_c(w, b, a, dz).start()

    def line_up(w):
        line = []
        for t in range(nz + 2):
            if 1 <= t < nz:
                line.append((step_z, (w, t)))
            if 0 <= t - 1 < nz:
                line += [(step_a, (w, a, t - 1)) for a in range(1, n)]
                line += [(step_b, (w, b, 0, t - 1)) for b in range(1, n)]
            if 0 <= t - 2 < nz:
                line += [(step_b, (w, b, a, t - 2)) for b in range(1, n) for a in range(1, n)]
        return line

    def take(line, most=1):
        for _ in range(min(most, len(line))):
            step, args = line.pop(0)
            step(*args)

    def phase_c(w):
        for b in range(n):
            for a in range(n):
                for dz in range(nz):
                    arrive_c(w, b, a, dz)

    def close(w):
        for dz in range(1, nz):
            copy_z(w, dz).wait_send()
        for dz in range(nz):
            for a in range(n):
                if a > 0:
                    copy_a(w, a, dz).wait_send()
                for b in range(n):
                    if b > 0:
                        copy_b(w, b, a, dz).wait_send()
                    copy_c(w, b, a, dz).wait_send()

    barrier = pltpu.get_barrier_semaphore()
    greeted = [((sp_me + j) % sp, dp_me) for j in range(1, sp)]
    greeted += [(sp_me, (y + j) % n * CORES + core) for j in range(1, n)]
    greeted += [partner]
    for device in greeted:
        pl.semaphore_signal(barrier, inc=1, device_id=device, device_id_type=MESH)
    pl.semaphore_wait(barrier, len(greeted))

    phase_own(0)
    phase_own(1)
    home = sp_me * dp + dp_me
    win[pl.ds(pl.multiple_of(home * rows, rows), rows), :] = win_ref[...]
    wout[:, pl.ds(pl.multiple_of(home * cols, cols), cols), :] = wout_ref[...]
    first, second = line_up(0), line_up(1)
    take(first, 2)

    share = LANES // heads
    count = channels // LANES
    wide = lanes // count

    step = jnp.exp(log_step_ref[...])
    lam_re, lam_im = lam_re_ref[...], lam_im_ref[...]
    decay_re, decay_im, ratio_re, ratio_im = step_factors(lam_re, lam_im, step)
    for row, table in enumerate((decay_re, decay_im, ratio_re, ratio_im)):
        for g in range(groups):
            factor[row : row + 1, g * states : (g + 1) * states] = table[g : g + 1, :]
    take(first, 2)
    for part, ref in enumerate((b_re_ref, b_im_ref, c_re_ref, c_im_ref)):
        for g in range(groups):
            compact[part, :, g * states : (g + 1) * states] = ref[g]
    take(first, 2)
    lane = lax.broadcasted_iota(jnp.int32, (heads, wide), 1)
    for i in range(count):
        for part in range(4):
            for level, value in enumerate(split(compact[part, :, i * wide : (i + 1) * wide])):
                for g in range(share):
                    inside = (lane >= g * states) & (lane < (g + 1) * states)
                    kept = jnp.where(inside, value, jnp.zeros_like(value))
                    tables[2 * part + level, i, g * heads : (g + 1) * heads, :] = kept
            if part % 2:
                take(first, 1)
    take(first, len(first))
    take(second, 2)
    phase_c(0)

    high_k = width // 4
    total = nn(x_ref[:, :high_k], win[:high_k, :])
    for i in range(1, 4):
        span = slice(i * high_k, (i + 1) * high_k)
        total += nn(x_ref[:, span], win[span, :])
        take(second, 1)
    inputs = total.astype(jnp.bfloat16)

    r = lax.broadcasted_iota(jnp.int32, (tokens, tokens), 0)
    c = lax.broadcasted_iota(jnp.int32, (tokens, tokens), 1)
    order = lambda v: (v & (SUBLANES - 1)) * steps + lax.shift_right_logical(v, 3)
    mix = jnp.where(c == order(r), 1.0, 0.0).astype(jnp.bfloat16)
    back = jnp.where(r == order(c), 1.0, 0.0).astype(jnp.bfloat16)
    source = nn(mix, inputs)
    spread = source.astype(jnp.bfloat16)

    decay = (factor[0:1, :], factor[1:2, :])
    ratio = (factor[2:3, :], factor[3:4, :])
    for i in range(count):
        span = slice(i * wide, (i + 1) * wide)
        piece = spread[:, i * LANES : (i + 1) * LANES]
        fed = tuple(nn(piece, tables[2 * part, i]) + nn(piece, tables[2 * part + 1, i]) for part in range(2))
        fed = cmul((ratio[0][:, span], ratio[1][:, span]), fed)
        drive[0, :, span] = fed[0]
        drive[1, :, span] = fed[1]
        shape = (SUBLANES, wide)
        mul = (jnp.broadcast_to(decay[0][:, span], shape), jnp.broadcast_to(decay[1][:, span], shape))
        state = (drive[0, :SUBLANES, span], drive[1, :SUBLANES, span])
        for k in range(1, steps):
            at = slice(k * SUBLANES, (k + 1) * SUBLANES)
            moved = cmul(mul, state)
            state = (moved[0] + drive[0, at, span], moved[1] + drive[1, at, span])
        ends[0, :, span] = state[0]
        ends[1, :, span] = state[1]
        take(second, 1)

    jump = cpow(decay, steps)
    carry = (ends[0, 0:1, :], ends[1, 0:1, :])
    for s in range(1, SUBLANES):
        moved = cmul(jump, carry)
        carry = (moved[0] + ends[0, s : s + 1, :], moved[1] + ends[1, s : s + 1, :])
    mine[0:1, :] = carry[0]
    mine[1:2, :] = carry[1]

    def exchange(j):
        return pltpu.make_async_remote_copy(
            src_ref=mine,
            dst_ref=others.at[j - 1],
            send_sem=send_e.at[j - 1],
            recv_sem=recv_e.at[j - 1],
            device_id=((sp_me + j) % sp, dp_me),
            device_id_type=MESH,
        )

    for j in range(1, sp):
        exchange(j).start()
    take(second, 2)
    far = cpow(decay, tokens)
    carry = (jnp.zeros_like(decay[0]), jnp.zeros_like(decay[0]))
    for j in range(1, sp):
        exchange(j).wait_recv()
    for j in range(sp - 1, 0, -1):
        moved = cmul(far, carry)
        before = sp_me >= j
        carry = (
            jnp.where(before, moved[0] + others[j - 1, 0:1, :], 0.0),
            jnp.where(before, moved[1] + others[j - 1, 1:2, :], 0.0),
        )
    edge[0, 0:1, :] = carry[0]
    edge[1, 0:1, :] = carry[1]
    for s in range(1, SUBLANES):
        moved = cmul(jump, carry)
        carry = (moved[0] + ends[0, s - 1 : s, :], moved[1] + ends[1, s - 1 : s, :])
        edge[0, s : s + 1, :] = carry[0]
        edge[1, s : s + 1, :] = carry[1]

    for i in range(count):
        span = slice(i * wide, (i + 1) * wide)
        shape = (SUBLANES, wide)
        mul = (jnp.broadcast_to(decay[0][:, span], shape), jnp.broadcast_to(decay[1][:, span], shape))
        state = (edge[0, :, span], edge[1, :, span])
        for k in range(steps):
            at = slice(k * SUBLANES, (k + 1) * SUBLANES)
            moved = cmul(mul, state)
            state = (moved[0] + drive[0, at, span], moved[1] + drive[1, at, span])
            drive[0, at, span] = state[0]
            drive[1, at, span] = state[1]
        summed = []
        for part in range(2):
            high, low = split(drive[part, :, span])
            c_high, c_low = tables[4 + 2 * part, i], tables[5 + 2 * part, i]
            summed.append(nt(high, c_high) + (nt(low, c_high) + nt(high, c_low)))
        here = slice(i * LANES, (i + 1) * LANES)
        result = jax.nn.gelu(summed[0] - summed[1] + skip_ref[:, here] * source[:, here])
        inner[:, here] = result.astype(jnp.bfloat16)
        take(second, 1)

    mixer_out = nn(back, inner[...]).astype(jnp.bfloat16)
    take(second, len(second))
    phase_c(1)
    tile = 2 * LANES
    for i in range(width // tile):
        span = slice(i * tile, (i + 1) * tile)
        linear = nt(mixer_out, wout[0, span, :])
        gate = nt(mixer_out, wout[1, span, :])
        out_ref[:, span] = (linear * jax.nn.sigmoid(gate)).astype(jnp.bfloat16)

    for j in range(1, sp):
        exchange(j).wait_send()
    close(0)
    close(1)


def shards(
    sizes,
    hidden_in,
    in_weight,
    lam_real,
    lam_imag,
    log_step,
    b_real,
    b_imag,
    c_real,
    c_imag,
    skip_weight,
    lin_weight,
    gate_weight,
):
    sp, dp = sizes
    n = dp // CORES
    nz = sp // n
    tokens, width = hidden_in.shape[1:]
    rows, channels = in_weight.shape
    groups, states, heads = b_real.shape
    lanes = groups * states
    pieces = jnp.stack((lin_weight.T, gate_weight.T), 0)
    count = channels // LANES
    bf16, f32 = jnp.bfloat16, jnp.float32
    pair = lambda *shape: [pltpu.SemaphoreType.DMA(shape)] * 2
    mixed = pl.pallas_call(
        functools.partial(kernel, sizes),
        out_shape=jax.ShapeDtypeStruct((tokens, width), bf16),
        in_specs=[pl.BlockSpec(memory_space=pltpu.VMEM)] * 11,
        out_specs=pl.BlockSpec(memory_space=pltpu.VMEM),
        scratch_shapes=[
            pltpu.VMEM((rows * sp * dp, channels), bf16),
            pltpu.VMEM((2, width, channels), bf16),
            pltpu.VMEM((8, count, LANES, lanes // count), bf16),
            pltpu.VMEM((4, lanes), f32),
            pltpu.VMEM((4, heads, lanes), f32),
            pltpu.VMEM((2, tokens, lanes), f32),
            pltpu.VMEM((2, SUBLANES, lanes), f32),
            pltpu.VMEM((2, SUBLANES, lanes), f32),
            pltpu.VMEM((2, lanes), f32),
            pltpu.VMEM((sp - 1, 2, lanes), f32),
            pltpu.VMEM((tokens, channels), bf16),
            *pair(2, nz - 1),
            *pair(2, n - 1, nz),
            *pair(2, n - 1, n, nz),
            *pair(2, n, n, nz),
            *pair(sp - 1),
        ],
        compiler_params=pltpu.CompilerParams(
            collective_id=0, has_side_effects=True, vmem_limit_bytes=60 * 1024 * 1024
        ),
    )(
        hidden_in[0],
        in_weight,
        pieces,
        lam_real,
        lam_imag,
        log_step[:, None],
        b_real.transpose(0, 2, 1),
        b_imag.transpose(0, 2, 1),
        c_real,
        c_imag,
        skip_weight[None],
    )
    return mixed[None]


def solution(mesh):
    sizes = (mesh.shape["sp"], mesh.shape["dp"])
    placed = (
        P("dp", "sp", None),
        P(("sp", "dp"), None),
        P(),
        P(),
        P(),
        P(),
        P(),
        P(),
        P(),
        P(),
        P(None, ("sp", "dp")),
        P(None, ("sp", "dp")),
    )
    return jax.shard_map(
        functools.partial(shards, sizes),
        mesh=mesh,
        in_specs=placed,
        out_specs=P("dp", "sp", None),
        check_vma=False,
    )
```
